256 devices in a mesh: kv: 32 (over z, x), tp: 8 (over y, core).
Axes of the slice: x: 4, y: 4, z: 8, core: 2. Of those that a mesh axis runs over, the one named last changes fastest.
Arguments:
- tokens: bfloat16 [32768, 2048], P('kv'), may hold values from -72 to 72
- query_weight: bfloat16 [2048, 2048], P(None, 'tp'), may hold values from -0.125 to 0.125
- key_projection_matrix: bfloat16 [2048, 1024], P(None, 'tp'), may hold values from -0.125 to 0.125
- value_projection_matrix: bfloat16 [2048, 1024], P(None, 'tp'), may hold values from -0.125 to 0.125
- out_weight: bfloat16 [2048, 2048], P('tp'), may hold values from -1.5 to 1.5
- chosen: int32 [256, 12], P('kv'), may hold values from -1 to 1023, as said below
Outputs:
- layer_out: bfloat16 [32768, 2048], P(('kv', 'tp'))
The draws below stay inside these ranges and needn't reach their ends.
Inputs may be any that keep to these rules, and one draw needn't show every extreme that they name: `chosen`: positions are grouped in consecutive groups of 1024. The blocks named in one row lie in distinct groups, all earlier than the group of the row's query block; a query block in group g has exactly min(12, g) entries that are not -1, first in its row, and the rest are -1. So the query blocks of one group name at most 8 blocks of any one other group, and in every draw some group's query blocks all name blocks of one same earlier group.
All inputs are finite; a program needn't handle non-finite values.
Results may differ from the reference program's by a relative error of at most 0.014.
The reference program's roundings to bfloat16 on the way count: a program that leaves them out, or rounds other values in their place, can miss the bound.
Values may be sent and summed in bfloat16 or wider, within the bound.
No kernel may reach another device: no remote copies, remote signals or barrier semaphores. Data moves between devices by JAX's collectives and lax.ppermute only.
A program may use at most 64 MiB of HBM per device.

```python
import jax
import jax.numpy as jnp
from jax import lax

MODEL_WIDTH = 2048
QUERY_HEADS = 16
KEY_VALUE_HEADS = 8
HEAD_SIZE = 128
TOK_DEV = 1024
QUERY_BLOCK_SPAN = 128
KEY_BLOCK_SPAN = 32
NFAR = 12
SEQUENCE_TOKENS = 32768
N_TP = 8


def draw_tokens(key, part):
    split_keys = jax.random.split(jax.random.fold_in(key, 11), 3)
    base_rows = jnp.clip(jax.random.normal(split_keys[0], (SEQUENCE_TOKENS, MODEL_WIDTH), jnp.float32), -6.0, 6.0)
    return base_rows.astype(jnp.bfloat16)


def draw_chosen(key, part):
    group_count = SEQUENCE_TOKENS // TOK_DEV
    per_group = TOK_DEV // QUERY_BLOCK_SPAN
    blocks_per_group = TOK_DEV // KEY_BLOCK_SPAN
    query_count = SEQUENCE_TOKENS // QUERY_BLOCK_SPAN
    split_keys = jax.random.split(jax.random.fold_in(key, 7), 4)
    owner_ids = jnp.arange(group_count, dtype=jnp.int32)
    home_group = jnp.arange(query_count, dtype=jnp.int32) // per_group
    first_local = jnp.arange(query_count, dtype=jnp.int32) % per_group == 0
    popular = jax.random.randint(split_keys[0], (group_count,), 0, 3) * (1 << 19)
    jitter = jax.random.randint(split_keys[1], (query_count, group_count), 0, 1 << 20)
    favoured = jax.random.randint(split_keys[2], (group_count,), 0, 1 << 20) % jnp.maximum(owner_ids, 1)
    source = home_group[:, None]
    target = owner_ids[None, :]
    forced = (target == favoured[home_group][:, None]) | first_local[:, None] & ((target == source - 1) | (target == source - group_count // 2))
    ranking = (jitter + popular[None, :]) * group_count + target
    ranking = jnp.where(forced, ranking + (1 << 29), ranking)
    ranking = jnp.where(target < source, ranking, -1)
    take_count = min(NFAR, group_count)
    best_scores, picked_owner = lax.top_k(ranking, take_count)
    inner_ids = jax.random.randint(split_keys[3], (query_count, take_count), 0, blocks_per_group)
    listed = jnp.where(best_scores >= 0, picked_owner.astype(jnp.int32) * blocks_per_group + inner_ids, -1)
    if take_count < NFAR:
        padding = jnp.full((query_count, NFAR - take_count), -1, jnp.int32)
        listed = jnp.concatenate([listed, padding], axis=1)
    return listed.astype(jnp.int32)


def steps_of(own_key, extent, cuts, smallest, high):
    def one(axis_at, shards_of):
        heights = jax.random.uniform(jax.random.fold_in(jax.random.fold_in(own_key, 6), axis_at), (shards_of,), jnp.float32, smallest / len(cuts), high / len(cuts))
        return jnp.repeat(jnp.exp(heights), extent[axis_at] // shards_of).reshape((-1,) + (1,) * (len(extent) - axis_at - 1))

    loudness = one(*cuts[0])
    for cut in cuts[1:]:
        loudness = loudness * one(*cut)
    return loudness


def bell_draw(rng, dims, scale, reach, pieces=(), kind=jnp.bfloat16):
    result = scale * jax.random.normal(rng, dims, jnp.float32)
    if pieces:
        result = result * steps_of(rng, dims, pieces, -0.22, 0.18)
    return jnp.clip(result, -reach, reach).astype(kind)


def setup_inputs(seed: int = 0) -> dict:
    arg_keys = jax.random.split(jax.random.key(seed), 7)
    return {
        "tokens": draw_tokens(jax.random.fold_in(arg_keys[6], 71), 0),
        "query_weight": bell_draw(arg_keys[1], (MODEL_WIDTH, QUERY_HEADS * HEAD_SIZE), MODEL_WIDTH ** -0.5, 0.125, ((1, 8),)),
        "key_projection_matrix": bell_draw(arg_keys[2], (MODEL_WIDTH, KEY_VALUE_HEADS * HEAD_SIZE), MODEL_WIDTH ** -0.5, 0.125, ((1, 8),)),
        "value_projection_matrix": bell_draw(arg_keys[3], (MODEL_WIDTH, KEY_VALUE_HEADS * HEAD_SIZE), MODEL_WIDTH ** -0.5, 0.125, ((1, 8),)),
        "out_weight": bell_draw(arg_keys[4], (QUERY_HEADS * HEAD_SIZE, MODEL_WIDTH), (HEAD_SIZE // 8) ** -0.5, 1.5, ((0, 8),)),
        "chosen": draw_chosen(jax.random.fold_in(arg_keys[6], 71), 0),
    }


def reference(tokens, query_weight, key_projection_matrix, value_projection_matrix, out_weight, chosen):
    queries = jnp.dot(tokens, query_weight, preferred_element_type=jnp.float32).astype(jnp.bfloat16)
    key_vectors = jnp.dot(tokens, key_projection_matrix, preferred_element_type=jnp.float32).astype(jnp.bfloat16)
    value_vectors = jnp.dot(tokens, value_projection_matrix, preferred_element_type=jnp.float32).astype(jnp.bfloat16)
    grouped_head_index = QUERY_HEADS // KEY_VALUE_HEADS
    diag_blocks = QUERY_BLOCK_SPAN // KEY_BLOCK_SPAN
    blocked_keys = key_vectors.reshape(SEQUENCE_TOKENS // KEY_BLOCK_SPAN, KEY_BLOCK_SPAN, KEY_VALUE_HEADS * HEAD_SIZE)
    blocked_values = value_vectors.reshape(SEQUENCE_TOKENS // KEY_BLOCK_SPAN, KEY_BLOCK_SPAN, KEY_VALUE_HEADS * HEAD_SIZE)
    offsets = jnp.arange(KEY_BLOCK_SPAN, dtype=jnp.int32)
    row_ids = jnp.arange(QUERY_BLOCK_SPAN, dtype=jnp.int32)

    def one_block(block_index):
        first_row = block_index * QUERY_BLOCK_SPAN
        queries_in_block = lax.dynamic_slice_in_dim(queries, first_row, QUERY_BLOCK_SPAN, 0)
        queries_in_block = queries_in_block.reshape(QUERY_BLOCK_SPAN, KEY_VALUE_HEADS, grouped_head_index, HEAD_SIZE).astype(jnp.float32)
        picked = lax.dynamic_slice_in_dim(chosen, block_index, 1, 0)[0]
        block_ids = jnp.concatenate([block_index * diag_blocks + jnp.arange(diag_blocks, dtype=jnp.int32), picked])
        is_valid = block_ids >= 0
        guarded_block_index = jnp.maximum(block_ids, 0)
        key_pos = (guarded_block_index[:, None] * KEY_BLOCK_SPAN + offsets[None, :]).reshape(-1)
        key_ok = jnp.broadcast_to(is_valid[:, None], (block_ids.shape[0], KEY_BLOCK_SPAN)).reshape(-1)
        query_pos = first_row + row_ids
        allowed = key_ok[None, :] & (key_pos[None, :] <= query_pos[:, None])
        nearby_keys = blocked_keys[guarded_block_index].reshape(-1, KEY_VALUE_HEADS, HEAD_SIZE).astype(jnp.float32)
        nearby_values = blocked_values[guarded_block_index].reshape(-1, KEY_VALUE_HEADS, HEAD_SIZE).astype(jnp.float32)
        scores = jnp.einsum("qgrd,kgd->grqk", queries_in_block, nearby_keys, precision=lax.Precision.HIGHEST) * (HEAD_SIZE ** -0.5)
        scores = jnp.where(allowed[None, None], scores, -jnp.inf)
        row_max = jnp.max(scores, axis=-1, keepdims=True)
        exp_scores = jnp.exp(scores - row_max)
        row_sum = jnp.sum(exp_scores, axis=-1, keepdims=True)
        weights = (exp_scores / row_sum).astype(jnp.bfloat16)
        mixed = jnp.einsum("grqk,kgd->qgrd", weights.astype(jnp.float32), nearby_values, precision=lax.Precision.HIGHEST)
        return mixed.astype(jnp.bfloat16).reshape(QUERY_BLOCK_SPAN, QUERY_HEADS * HEAD_SIZE)

    all_blocks = lax.map(one_block, jnp.arange(SEQUENCE_TOKENS // QUERY_BLOCK_SPAN, dtype=jnp.int32))
    attended = all_blocks.reshape(SEQUENCE_TOKENS, QUERY_HEADS * HEAD_SIZE)
    slice_width = QUERY_HEADS * HEAD_SIZE // N_TP
    summed = jnp.zeros((SEQUENCE_TOKENS, MODEL_WIDTH), jnp.float32)
    for part_index in range(N_TP):
        lower = part_index * slice_width
        partial_value = jnp.dot(attended[:, lower:lower + slice_width], out_weight[lower:lower + slice_width],
                          preferred_element_type=jnp.float32)
        rounded = lax.optimization_barrier(partial_value.astype(jnp.bfloat16))
        summed = summed + rounded.astype(jnp.float32)
    return summed.astype(jnp.bfloat16)
```

```python
import jax
import jax.numpy as jnp
from jax import lax
from jax.experimental import pallas as pl
from jax.experimental.pallas import tpu as pltpu
from jax.sharding import PartitionSpec as P

HEAD = 128
QB = 128
KB = 32
NFAR = 12
NX = 4
NZ = 8
NY = 4
BF = jnp.bfloat16
F32 = jnp.float32
NT = (((1,), (1,)), ((), ()))


CORES = [(t, t ^ 1) for t in range(2 * NY)]


def along_z(k):
    return [(z * NX + x, (z + k) % NZ * NX + x) for z in range(NZ) for x in range(NX)]


def along_x(k):
    return [(z * NX + x, z * NX + (x + k) % NX) for z in range(NZ) for x in range(NX)]


def along_y(k):
    return [(y * 2 + c, (y + k) % NY * 2 + c) for y in range(NY) for c in range(2)]


def dot(a, b):
    return jnp.dot(a, b, preferred_element_type=F32)


VMEM = pl.BlockSpec(memory_space=pltpu.VMEM)
SMEM = pl.BlockSpec(memory_space=pltpu.SMEM)


def params(mib):
    return pltpu.CompilerParams(vmem_limit_bytes=mib * 1024 * 1024)


def pick_body(count):
    def body(want, *refs):
        ins, outs = refs[: 2 * count], refs[2 * count :]

        def step(j, carry):
            for d in range(count):
                for r in range(NX):
                    b = pl.multiple_of(want[r, d * 8 + j] * KB, KB)
                    for s in range(2):
                        outs[r][d, s, j] = ins[2 * d + s][pl.ds(b, KB), :]
            return carry

        lax.fori_loop(0, 8, step, 0)

    return body


def pick(want, pairs):
    count = len(pairs)
    return pl.pallas_call(
        pick_body(count),
        out_shape=[jax.ShapeDtypeStruct((count, 2, 8, KB, HEAD), BF)] * NX,
        in_specs=[SMEM] + [VMEM] * (2 * count),
        out_specs=[VMEM] * NX,
        compiler_params=params(8),
        cost_estimate=pl.CostEstimate(
            flops=4_000_000 * count, bytes_accessed=1_000_000 * count, transcendentals=0
        ),
    )(want, *[a for p in pairs for a in p])


def attend_body(counts):
    def body(place, named, q, k, v, *refs):
        recv, (out, kbuf, vbuf) = refs[:-3], refs[-3:]
        far = NFAR * KB
        row = lax.broadcasted_iota(jnp.int32, (2 * QB, QB), 0) % QB
        col = lax.broadcasted_iota(jnp.int32, (2 * QB, QB), 1)
        causal = jnp.where(col <= row, 0.0, -jnp.inf).astype(F32)
        scale = HEAD ** (-0.5)

        def step(j, carry):
            at = pl.multiple_of(j * QB, QB)
            vbuf[...] = jnp.zeros_like(vbuf)
            slot = 0
            for b, count in enumerate(counts):
                for d in range(count):
                    for r in range(NX):
                        p = pl.multiple_of(place[j, slot] * KB, KB)
                        kbuf[pl.ds(p, KB), :] = recv[NX * b + r][d, 0, j]
                        vbuf[pl.ds(p, KB), :] = recv[NX * b + r][d, 1, j]
                        slot += 1
            fcol = lax.broadcasted_iota(jnp.int32, (1, far), 1)
            bias = jnp.where(fcol < named[j] * KB, 0.0, -jnp.inf).astype(F32)
            qq = jnp.concatenate([q[pl.ds(at, QB), :HEAD], q[pl.ds(at, QB), HEAD:]], axis=0)
            own = lax.dot_general(qq, k[pl.ds(at, QB), :], NT, preferred_element_type=F32)
            oth = lax.dot_general(qq, kbuf[:far, :], NT, preferred_element_type=F32)
            own = own * scale + causal
            oth = oth * scale + bias
            top = jnp.maximum(jnp.max(own, axis=1, keepdims=True), jnp.max(oth, axis=1, keepdims=True))
            own = jnp.exp(own - top)
            oth = jnp.exp(oth - top)
            total = jnp.sum(own, axis=1, keepdims=True) + jnp.sum(oth, axis=1, keepdims=True)
            inv = 1.0 / total
            mixed = dot((own * inv).astype(BF), v[pl.ds(at, QB), :])
            mixed = (mixed + dot((oth * inv).astype(BF), vbuf[:far, :])).astype(BF)
            out[pl.ds(at, QB), :HEAD] = mixed[:QB]
            out[pl.ds(at, QB), HEAD:] = mixed[QB:]
            return carry

        lax.fori_loop(0, q.shape[0] // QB, step, 0)

    return body


def attend(place, named, q, k, v, recv):
    counts = [r[0].shape[0] for r in recv]
    return pl.pallas_call(
        attend_body(counts),
        out_shape=jax.ShapeDtypeStruct(q.shape, BF),
        in_specs=[SMEM, SMEM] + [VMEM] * (3 + NX * len(recv)),
        out_specs=VMEM,
        scratch_shapes=[pltpu.VMEM(((NFAR + 1) * KB, HEAD), BF)] * 2,
        compiler_params=params(16),
        cost_estimate=pl.CostEstimate(
            flops=600_000_000, bytes_accessed=6_000_000, transcendentals=1_000_000
        ),
        name="attend",
    )(place, named, q, k, v, *[a for r in recv for a in r])


def project_body(spot, att, *refs):
    weights, out = refs[:-1], refs[-1]
    tile = 256

    def step(n, carry):
        cols = pl.ds(pl.multiple_of(n * tile, tile), tile)
        acc = jnp.zeros((QB, tile), F32)
        for core in range(2):
            w0, wm, wp, top, low = weights[5 * core : 5 * core + 5]
            for i, w in enumerate((w0, wm, wp)):
                acc += dot(att[spot[core, i]], w[:, cols]).astype(BF).astype(F32)
            a = att[spot[core, 3]]
            part = dot(a[:, :HEAD], top[:, cols]) + dot(a[:, HEAD:], low[:, cols])
            acc += part.astype(BF).astype(F32)
        out[:, cols] = acc.astype(BF)
        return carry

    lax.fori_loop(0, out.shape[1] // tile, step, 0)


def project(spot, att, weights):
    width = weights[0].shape[1]
    return pl.pallas_call(
        project_body,
        out_shape=jax.ShapeDtypeStruct((QB, width), BF),
        in_specs=[SMEM] + [VMEM] * (1 + len(weights)),
        out_specs=VMEM,
        compiler_params=params(14),
        cost_estimate=pl.CostEstimate(
            flops=1_000_000_000, bytes_accessed=9_000_000, transcendentals=0
        ),
        name="project",
    )(spot, att, *weights)


def layer(tokens, wq, wk, wv, wo, chosen):
    me = lax.axis_index("kv")
    z, x = me // NX, me % NX
    tp = lax.axis_index("tp")
    per = tokens.shape[0] // KB

    lists = [chosen] + [lax.ppermute(chosen, "kv", along_x(-r)) for r in range(1, NX)]
    k = dot(tokens, wk).astype(BF)
    v = dot(tokens, wv).astype(BF)

    dist = jnp.arange(NZ, dtype=jnp.int32)
    step_x = jnp.arange(NX, dtype=jnp.int32)
    home = (z - dist) % NZ * NX
    lists = jnp.stack(lists)[:, None]
    mine = lists // per == (home + x)[None, :, None, None]
    want = jnp.sum(jnp.where(mine, lists % per, 0), axis=3)
    source = home[:, None] + (x - step_x) % NX
    here = chosen[:, None, None, :] // per == source[None, :, :, None]
    order = jnp.arange(NFAR, dtype=jnp.int32) - NFAR
    place = NFAR + jnp.sum(jnp.where(here, order, 0), axis=3)
    named = jnp.sum((chosen >= 0).astype(jnp.int32), axis=1)

    up, down = along_z(1), along_z(-1)
    got_k, got_v = {0: k}, {0: v}
    uk, uv, dk, dv = k, v, k, v
    for step in range(1, NZ // 2 + 1):
        uk = got_k[step] = lax.ppermute(uk, "kv", up)
        if step < NZ // 2:
            dk = got_k[NZ - step] = lax.ppermute(dk, "kv", down)
            uv = got_v[step] = lax.ppermute(uv, "kv", up)
        dv = got_v[NZ - step] = lax.ppermute(dv, "kv", down)

    batches = [[0]] + [[s, NZ - s] for s in range(1, NZ // 2)] + [[NZ // 2]]
    recv = []
    for batch in batches:
        rows = jnp.concatenate([want[:, d] for d in batch], axis=1)
        sent = pick(rows, [(got_k[d], got_v[d]) for d in batch])
        recv.append([sent[0]] + [lax.ppermute(sent[r], "kv", along_x(r)) for r in range(1, NX)])
    spots = jnp.concatenate([place[:, d] for batch in batches for d in batch], axis=1)

    wm = lax.ppermute(wo, "tp", along_y(1))
    wp = lax.ppermute(wo, "tp", along_y(-1))
    top = lax.ppermute(wm[:HEAD], "tp", along_y(1))
    low = lax.ppermute(wp[HEAD:], "tp", along_y(-1))
    weights = [wo, wm, wp, top, low]
    weights += [lax.ppermute(w, "tp", CORES) for w in weights]

    q = dot(tokens, wq).astype(BF)
    mixed = attend(spots, named, q, k, v, recv)
    att = lax.all_to_all(mixed.reshape(2 * NY, QB, -1), "tp", 0, 0, tiled=True)
    y, c = tp // 2, tp % 2
    rows = jnp.stack([y, (y - 1) % NY, (y + 1) % NY, (y + 2) % NY]) * 2
    return project(jnp.stack([rows + c, rows + 1 - c]), att, weights)


def solution(mesh):
    return jax.shard_map(
        layer,
        mesh=mesh,
        in_specs=(
            P("kv", None),
            P(None, "tp"),
            P(None, "tp"),
            P(None, "tp"),
            P("tp", None),
            P("kv", None),
        ),
        out_specs=P(("kv", "tp"), None),
        check_vma=False,
    )
```

```python
import jax
import jax.numpy as jnp
import numpy as np
from jax import lax
from jax.experimental import pallas as pl
from jax.experimental.pallas import tpu as pltpu
from jax.sharding import PartitionSpec as P

HEAD = 128
QB = 128
KB = 32
NFAR = 12
NX = 4
NZ = 8
NY = 4
GROUP = 4
BF = jnp.bfloat16
F32 = jnp.float32
NT = (((1,), (1,)), ((), ()))


CORES = [(t, t ^ 1) for t in range(2 * NY)]


def along_z(k):
    return [(z * NX + x, (z + k) % NZ * NX + x) for z in range(NZ) for x in range(NX)]


def along_x(k):
    return [(z * NX + x, z * NX + (x + k) % NX) for z in range(NZ) for x in range(NX)]


def across(r):
    return [(z * NX + x, (z + 1) % NZ * NX + (x + r) % NX) for z in range(NZ) for x in range(NX)]


def along_y(k):
    return [(y * 2 + c, (y + k) % NY * 2 + c) for y in range(NY) for c in range(2)]


def dot(a, b):
    return jnp.dot(a, b, preferred_element_type=F32)


VMEM = pl.BlockSpec(memory_space=pltpu.VMEM)
SMEM = pl.BlockSpec(memory_space=pltpu.SMEM)
ANY = pl.BlockSpec(memory_space=pl.ANY)


def params(mib):
    return pltpu.CompilerParams(vmem_limit_bytes=mib * 1024 * 1024)


def rows_body(count, parts):
    def body(tok, *refs):
        weights, (out, t, w, sems) = refs[:count], refs[count:]
        tile = out.shape[0] // parts
        wide = out.shape[1] // count
        copies = [
            pltpu.make_async_copy(ref, w.at[:, pl.ds(n * wide, wide)], sems.at[n])
            for n, ref in enumerate(weights)
        ]
        blocks = [pl.ds(n * tile, tile) for n in range(parts)]
        copies += [
            pltpu.make_async_copy(tok.at[b], t.at[b], sems.at[count + n]) for n, b in enumerate(blocks)
        ]
        for c in copies:
            c.start()
        for c in copies[:count]:
            c.wait()
        for c, b in zip(copies[count:], blocks):
            c.wait()
            out[b, :] = dot(t[b, :], w[...]).astype(BF)

    return body


def rows_project(tokens, weights, limit):
    rows, width = tokens.shape
    parts = 4
    total = sum(w.shape[1] for w in weights)
    return pl.pallas_call(
        rows_body(len(weights), parts),
        out_shape=jax.ShapeDtypeStruct((rows, total), BF),
        in_specs=[ANY] * (1 + len(weights)),
        out_specs=VMEM,
        scratch_shapes=[
            pltpu.VMEM((rows, width), BF),
            pltpu.VMEM((width, total), BF),
            pltpu.SemaphoreType.DMA((len(weights) + parts,)),
        ],
        compiler_params=params(limit),
        cost_estimate=pl.CostEstimate(
            flops=1_000_000_000, bytes_accessed=6_000_000, transcendentals=0
        ),
    )(tokens, *weights)


def pick_body(first, count, offsets):
    def body(want, *refs):
        ins, outs = refs[:count], refs[count:]

        def step(j, carry):
            for d in range(count):
                for out, r in zip(outs, offsets):
                    b = pl.multiple_of(want[r, (first + d) * 8 + j] * KB, KB)
                    out[d, j] = ins[d][pl.ds(b, KB), :]
            return carry

        lax.fori_loop(0, 8, step, 0)

    return body


def pick(want, first, held, offsets):
    count = len(held)
    return pl.pallas_call(
        pick_body(first, count, offsets),
        out_shape=[jax.ShapeDtypeStruct((count, 8, KB, 2 * HEAD), BF)] * len(offsets),
        in_specs=[SMEM] + [VMEM] * count,
        out_specs=[VMEM] * len(offsets),
        compiler_params=params(6),
        cost_estimate=pl.CostEstimate(
            flops=4_000_000 * count, bytes_accessed=1_000_000 * count, transcendentals=0
        ),
    )(want, *held)


def gather_blocks(kv, want, held, recv, counts, first, last, j):
    slot = 0
    source = 0

    def put(block):
        nonlocal slot
        kv[slot * KB : (slot + 1) * KB, :] = block
        slot += 1

    for b, count in enumerate(counts):
        for d in range(count):
            mine = pl.multiple_of(want[0, (first + source) * 8 + j] * KB, KB)
            put(held[source][pl.ds(mine, KB), :])
            for r in range(1, NX):
                put(recv[(NX - 1) * b + r - 1][d, j])
            source += 1
    for r in range(last):
        put(recv[(NX - 1) * len(counts) + r][0, j])


def both_heads(q, at):
    return jnp.concatenate([q[pl.ds(at, QB), :HEAD], q[pl.ds(at, QB), HEAD:]], axis=0)


def row_max(a):
    return jnp.max(a, axis=1, keepdims=True)


def row_sum(a):
    return jnp.sum(a, axis=1, keepdims=True)


def places(g, n):
    j = g * GROUP + n
    return j, pl.multiple_of(j * QB, QB), pl.ds(pl.multiple_of(j * 2 * QB, 2 * QB), 2 * QB)


def early_body(counts):
    total = sum(counts)
    far = total * NX * KB

    def body(want, bias, q, *refs):
        held, recv = refs[:total], refs[total:-4]
        acc, top, low, kv = refs[-4:]
        row = lax.broadcasted_iota(jnp.int32, (2 * QB, QB), 0) % QB
        col = lax.broadcasted_iota(jnp.int32, (2 * QB, QB), 1)
        causal = jnp.where(col <= row, 0.0, -jnp.inf).astype(F32)
        scale = HEAD ** (-0.5)

        def step(g, carry):
            spots = [places(g, n) for n in range(GROUP)]
            own, oth, m = [], [], []
            for n, (j, at, to) in enumerate(spots):
                gather_blocks(kv.at[n], want, held, recv, counts, 0, 0, j)
            for n, (j, at, to) in enumerate(spots):
                qq = both_heads(q, at)
                mine = held[0][pl.ds(at, QB), :HEAD]
                own.append(lax.dot_general(qq, mine, NT, preferred_element_type=F32) * scale + causal)
                theirs = kv[n, :, :HEAD]
                oth.append(
                    lax.dot_general(qq, theirs, NT, preferred_element_type=F32) * scale
                    + bias[pl.ds(j, 1), :far]
                )
            for n in range(GROUP):
                m.append(jnp.maximum(row_max(own[n]), row_max(oth[n])))
            for n in range(GROUP):
                own[n] = jnp.exp(own[n] - m[n])
                oth[n] = jnp.exp(oth[n] - m[n])
            for n, (j, at, to) in enumerate(spots):
                top[to, :] = jnp.broadcast_to(m[n], (2 * QB, HEAD))
                low[to, :] = jnp.broadcast_to(row_sum(own[n]) + row_sum(oth[n]), (2 * QB, HEAD))
                mixed = dot(own[n].astype(BF), held[0][pl.ds(at, QB), HEAD:])
                acc[to, :] = mixed + dot(oth[n].astype(BF), kv[n, :, HEAD:])
            return carry

        lax.fori_loop(0, q.shape[0] // QB // GROUP, step, 0)

    return body


def late_body(counts, first, last):
    total = sum(counts)

    def body(want, bias, q, acc, top, low, *refs):
        held, recv = refs[:total], refs[total:-2]
        out, kv = refs[-2:]
        begin = first * NX * KB
        far = kv.shape[1]
        scale = HEAD ** (-0.5)

        def step(g, carry):
            spots = [places(g, n) for n in range(GROUP)]
            oth, m, keep, inv = [], [], [], []
            for n, (j, at, to) in enumerate(spots):
                gather_blocks(kv.at[n], want, held, recv, counts, first, last, j)
            for n, (j, at, to) in enumerate(spots):
                part = lax.dot_general(both_heads(q, at), kv[n, :, :HEAD], NT, preferred_element_type=F32)
                oth.append(part * scale + bias[pl.ds(j, 1), begin : begin + far])
            for n, (j, at, to) in enumerate(spots):
                m.append(jnp.maximum(top[to, :], row_max(oth[n])))
            for n, (j, at, to) in enumerate(spots):
                oth[n] = jnp.exp(oth[n] - jnp.concatenate([m[n]] * (far // HEAD), axis=1))
                keep.append(jnp.exp(top[to, :] - m[n]))
            for n, (j, at, to) in enumerate(spots):
                inv.append(1.0 / (low[to, :] * keep[n] + row_sum(oth[n])))
            for n, (j, at, to) in enumerate(spots):
                mixed = acc[to, :] * keep[n] + dot(oth[n].astype(BF), kv[n, :, HEAD:])
                mixed = (mixed * inv[n]).astype(BF)
                out[pl.ds(at, QB), :HEAD] = mixed[:QB]
                out[pl.ds(at, QB), HEAD:] = mixed[QB:]
            return carry

        lax.fori_loop(0, q.shape[0] // QB // GROUP, step, 0)

    return body


def attend_early(want, bias, q, held, recv):
    counts = [r[0].shape[0] for r in recv]
    ins = [*held, *[a for r in recv for a in r]]
    rows = 2 * q.shape[0]
    return pl.pallas_call(
        early_body(counts),
        out_shape=[
            jax.ShapeDtypeStruct((rows, HEAD), F32),
            jax.ShapeDtypeStruct((rows, HEAD), F32),
            jax.ShapeDtypeStruct((rows, HEAD), F32),
        ],
        in_specs=[SMEM] + [VMEM] * (2 + len(ins)),
        out_specs=[VMEM] * 3,
        scratch_shapes=[pltpu.VMEM((GROUP, sum(counts) * NX * KB, 2 * HEAD), BF)],
        compiler_params=params(16),
        cost_estimate=pl.CostEstimate(
            flops=900_000_000, bytes_accessed=6_000_000, transcendentals=1_600_000
        ),
        name="early",
    )(want, bias, q, *ins)


def attend_late(want, bias, q, sums, held, recv, last):
    counts = [r[0].shape[0] for r in recv]
    first = bias.shape[1] // (NX * KB) - sum(counts) - 1
    ins = [*held, *[a for r in recv for a in r], *last]
    return pl.pallas_call(
        late_body(counts, first, len(last)),
        out_shape=jax.ShapeDtypeStruct(q.shape, BF),
        in_specs=[SMEM] + [VMEM] * (2 + len(sums) + len(ins)),
        out_specs=VMEM,
        scratch_shapes=[pltpu.VMEM((GROUP, (sum(counts) + 1) * NX * KB, 2 * HEAD), BF)],
        compiler_params=params(16),
        cost_estimate=pl.CostEstimate(
            flops=400_000_000, bytes_accessed=6_000_000, transcendentals=800_000
        ),
        name="late",
    )(want, bias, q, *sums, *ins)


def project_body(spot, att, *refs):
    count = 2 * NY
    weights, (out, near, acc, sems) = refs[:count], refs[count:]
    copies = [pltpu.make_async_copy(w, near.at[i], sems.at[i]) for i, w in enumerate(weights)]
    for c in copies:
        c.start()
    tile = 512
    for i, c in enumerate(copies):
        c.wait()
        mine = att[spot[i // NY, i % NY]]
        for n in range(out.shape[1] // tile):
            cols = slice(n * tile, (n + 1) * tile)
            part = dot(mine, near[i, :, cols]).astype(BF).astype(F32)
            if i == 0:
                acc[:, cols] = part
            elif i < count - 1:
                acc[:, cols] += part
            else:
                out[:, cols] = (acc[:, cols] + part).astype(BF)


def project(spot, att, weights):
    deep, width = weights[0].shape
    return pl.pallas_call(
        project_body,
        out_shape=jax.ShapeDtypeStruct((QB, width), BF),
        in_specs=[SMEM, VMEM] + [ANY] * len(weights),
        out_specs=VMEM,
        scratch_shapes=[
            pltpu.VMEM((len(weights), deep, width), BF),
            pltpu.VMEM((QB, width), F32),
            pltpu.SemaphoreType.DMA((len(weights),)),
        ],
        compiler_params=params(14),
        cost_estimate=pl.CostEstimate(
            flops=1_000_000_000, bytes_accessed=9_000_000, transcendentals=0
        ),
        name="project",
    )(spot, att, *weights)


def layer(tokens, wq, wk, wv, wo, chosen):
    me = lax.axis_index("kv")
    z, x = me // NX, me % NX
    tp = lax.axis_index("tp")
    per = tokens.shape[0] // KB

    kv = rows_project(tokens, (wk, wv), 60)

    row = jnp.stack([chosen] + [lax.ppermute(chosen, "kv", along_x(-r)) for r in range(1, NX)])
    above = lax.ppermute(row, "kv", along_z(-1))

    order = [0, *[d for s in range(1, NZ // 2) for d in (s, NZ - s)], NZ // 2]

    def wants(lists, dist):
        groups = (z - np.repeat(np.array(dist, np.int32), chosen.shape[0])) % NZ * NX + x
        named = jnp.concatenate([lists] * len(dist), axis=1)
        mine = named // per == groups[None, :, None]
        return jnp.sum(jnp.where(mine, named % per, 0), axis=2)

    want = wants(row, order[:-1])
    want_above = wants(above, [NZ // 2 - 1])
    dist = np.repeat(np.array(order, np.int32), NX * KB)
    beyond = np.tile(np.repeat(np.arange(NX, dtype=np.int32), KB), NZ)
    source = (z - dist) % NZ * NX + (x - beyond) % NX
    groups = chosen // per
    here = groups[:, :1] == source[None, :]
    for n in range(1, NFAR):
        here = here | (groups[:, n : n + 1] == source[None, :])
    bias = jnp.where(here, 0.0, -jnp.inf).astype(F32)

    held = {0: kv}
    up = down = kv
    for step in range(1, NZ // 2):
        up = held[step] = lax.ppermute(up, "kv", along_z(1))
        down = held[NZ - step] = lax.ppermute(down, "kv", along_z(-1))

    recv = []
    batches = [[0, 1, NZ - 1]] + [[s, NZ - s] for s in range(2, NZ // 2)]
    beside = range(1, NX)
    for batch in batches:
        sent = pick(want, order.index(batch[0]), [held[d] for d in batch], beside)
        recv.append([lax.ppermute(a, "kv", along_x(r)) for a, r in zip(sent, beside)])
    sent = pick(want_above, 0, [held[NZ // 2 - 1]], range(NX))
    last = [lax.ppermute(a, "kv", across(r)) for r, a in enumerate(sent)]

    wm = lax.ppermute(wo, "tp", along_y(1))
    wp = lax.ppermute(wo, "tp", along_y(-1))
    weights = [wo, wm, wp, lax.ppermute(wm, "tp", along_y(1))]
    weights += [lax.ppermute(w, "tp", CORES) for w in weights]

    q = rows_project(tokens, (wq,), 60)
    line = [held[d] for d in order[:-1]]
    cut = len(line) - len(batches[-1])
    sums = attend_early(want, bias, q, line[:cut], recv[:-1])
    mixed = attend_late(want, bias, q, sums, line[cut:], recv[-1:], last)
    att = lax.all_to_all(mixed.reshape(2 * NY, QB, -1), "tp", 0, 0, tiled=True)
    y, c = tp // 2, tp % 2
    rows = jnp.stack([y, (y - 1) % NY, (y + 1) % NY, (y + 2) % NY]) * 2
    return project(jnp.stack([rows + c, rows + 1 - c]), att, weights)


def solution(mesh):
    return jax.shard_map(
        layer,
        mesh=mesh,
        in_specs=(
            P("kv", None),
            P(None, "tp"),
            P(None, "tp"),
            P(None, "tp"),
            P("tp", None),
            P("kv", None),
        ),
        out_specs=P(("kv", "tp"), None),
        check_vma=False,
    )
```

```python
import jax
import jax.numpy as jnp
import numpy as np
from jax import lax
from jax.experimental import pallas as pl
from jax.experimental.pallas import tpu as pltpu
from jax.sharding import PartitionSpec as P

HEAD = 128
QB = 128
KB = 32
NFAR = 12
NX = 4
NZ = 8
NY = 4
GROUP = 4
BF = jnp.bfloat16
F32 = jnp.float32
NT = (((1,), (1,)), ((), ()))


CORES = [(t, t ^ 1) for t in range(2 * NY)]


def along_z(k):
    return [(z * NX + x, (z + k) % NZ * NX + x) for z in range(NZ) for x in range(NX)]


def along_x(k):
    return [(z * NX + x, z * NX + (x + k) % NX) for z in range(NZ) for x in range(NX)]


def along_y(k):
    return [(y * 2 + c, (y + k) % NY * 2 + c) for y in range(NY) for c in range(2)]


def dot(a, b):
    return jnp.dot(a, b, preferred_element_type=F32)


VMEM = pl.BlockSpec(memory_space=pltpu.VMEM)
SMEM = pl.BlockSpec(memory_space=pltpu.SMEM)
ANY = pl.BlockSpec(memory_space=pl.ANY)


def params(mib):
    return pltpu.CompilerParams(vmem_limit_bytes=mib * 1024 * 1024)


def rows_body(count, parts):
    def body(tok, *refs):
        weights, (out, t, w, sems) = refs[:count], refs[count:]
        tile = out.shape[0] // parts
        wide = out.shape[1] // count
        copies = [
            pltpu.make_async_copy(ref, w.at[:, pl.ds(n * wide, wide)], sems.at[n])
            for n, ref in enumerate(weights)
        ]
        blocks = [pl.ds(n * tile, tile) for n in range(parts)]
        copies += [
            pltpu.make_async_copy(tok.at[b], t.at[b], sems.at[count + n]) for n, b in enumerate(blocks)
        ]
        for c in copies:
            c.start()
        for c in copies[:count]:
            c.wait()
        for c, b in zip(copies[count:], blocks):
            c.wait()
            out[b, :] = dot(t[b, :], w[...]).astype(BF)

    return body


def rows_project(tokens, weights, limit):
    rows, width = tokens.shape
    parts = 4
    total = sum(w.shape[1] for w in weights)
    return pl.pallas_call(
        rows_body(len(weights), parts),
        out_shape=jax.ShapeDtypeStruct((rows, total), BF),
        in_specs=[ANY] * (1 + len(weights)),
        out_specs=VMEM,
        scratch_shapes=[
            pltpu.VMEM((rows, width), BF),
            pltpu.VMEM((width, total), BF),
            pltpu.SemaphoreType.DMA((len(weights) + parts,)),
        ],
        compiler_params=params(limit),
        cost_estimate=pl.CostEstimate(
            flops=1_000_000_000, bytes_accessed=6_000_000, transcendentals=0
        ),
    )(tokens, *weights)


def pick_body(first, count, offsets):
    def body(want, *refs):
        ins, outs = refs[:count], refs[count:]

        def step(j, carry):
            for d in range(count):
                for out, r in zip(outs, offsets):
                    b = pl.multiple_of(want[r, (first + d) * 8 + j] * KB, KB)
                    out[d, j] = ins[d][pl.ds(b, KB), :]
            return carry

        lax.fori_loop(0, 8, step, 0)

    return body


def pick(want, first, held, offsets):
    count = len(held)
    return pl.pallas_call(
        pick_body(first, count, offsets),
        out_shape=[jax.ShapeDtypeStruct((count, 8, KB, 2 * HEAD), BF)] * len(offsets),
        in_specs=[SMEM] + [VMEM] * count,
        out_specs=[VMEM] * len(offsets),
        compiler_params=params(6),
        cost_estimate=pl.CostEstimate(
            flops=4_000_000 * count, bytes_accessed=1_000_000 * count, transcendentals=0
        ),
    )(want, *held)


def gather_blocks(kv, want, held, recv, counts, first, j):
    slot = 0
    source = 0

    def put(block):
        nonlocal slot
        kv[slot * KB : (slot + 1) * KB, :] = block
        slot += 1

    for b, count in enumerate(counts):
        for d in range(count):
            mine = pl.multiple_of(want[0, (first + source) * 8 + j] * KB, KB)
            put(held[source][pl.ds(mine, KB), :])
            for r in range(1, NX):
                put(recv[(NX - 1) * b + r - 1][d, j])
            source += 1


def both_heads(q, at):
    return jnp.concatenate([q[pl.ds(at, QB), :HEAD], q[pl.ds(at, QB), HEAD:]], axis=0)


def row_max(a):
    return jnp.max(a, axis=1, keepdims=True)


def row_sum(a):
    return jnp.sum(a, axis=1, keepdims=True)


def places(g, n):
    j = g * GROUP + n
    return j, pl.multiple_of(j * QB, QB), pl.ds(pl.multiple_of(j * 2 * QB, 2 * QB), 2 * QB)


def early_body(counts):
    total = sum(counts)
    far = total * NX * KB

    def body(want, bias, q, *refs):
        held, recv = refs[:total], refs[total:-4]
        acc, top, low, kv = refs[-4:]
        row = lax.broadcasted_iota(jnp.int32, (2 * QB, QB), 0) % QB
        col = lax.broadcasted_iota(jnp.int32, (2 * QB, QB), 1)
        causal = jnp.where(col <= row, 0.0, -jnp.inf).astype(F32)
        scale = HEAD ** (-0.5)

        def step(g, carry):
            spots = [places(g, n) for n in range(GROUP)]
            own, oth, m = [], [], []
            for n, (j, at, to) in enumerate(spots):
                gather_blocks(kv.at[n], want, held, recv, counts, 0, j)
            for n, (j, at, to) in enumerate(spots):
                qq = both_heads(q, at)
                mine = held[0][pl.ds(at, QB), :HEAD]
                own.append(lax.dot_general(qq, mine, NT, preferred_element_type=F32) * scale + causal)
                theirs = kv[n, :, :HEAD]
                oth.append(
                    lax.dot_general(qq, theirs, NT, preferred_element_type=F32) * scale
                    + bias[pl.ds(j, 1), :far]
                )
            for n in range(GROUP):
                m.append(jnp.maximum(row_max(own[n]), row_max(oth[n])))
            for n in range(GROUP):
                own[n] = jnp.exp(own[n] - m[n])
                oth[n] = jnp.exp(oth[n] - m[n])
            for n, (j, at, to) in enumerate(spots):
                top[to, :] = jnp.broadcast_to(m[n], (2 * QB, HEAD))
                low[to, :] = jnp.broadcast_to(row_sum(own[n]) + row_sum(oth[n]), (2 * QB, HEAD))
                mixed = dot(own[n].astype(BF), held[0][pl.ds(at, QB), HEAD:])
                acc[to, :] = mixed + dot(oth[n].astype(BF), kv[n, :, HEAD:])
            return carry

        lax.fori_loop(0, q.shape[0] // QB // GROUP, step, 0)

    return body


def late_body(counts, first):
    total = sum(counts)

    def body(want, bias, q, acc, top, low, *refs):
        held, recv = refs[:total], refs[total:-2]
        out, kv = refs[-2:]
        begin = first * NX * KB
        far = kv.shape[1]
        scale = HEAD ** (-0.5)

        def step(g, carry):
            spots = [places(g, n) for n in range(GROUP)]
            oth, m, keep, inv = [], [], [], []
            for n, (j, at, to) in enumerate(spots):
                gather_blocks(kv.at[n], want, held, recv, counts, first, j)
            for n, (j, at, to) in enumerate(spots):
                part = lax.dot_general(both_heads(q, at), kv[n, :, :HEAD], NT, preferred_element_type=F32)
                oth.append(part * scale + bias[pl.ds(j, 1), begin : begin + far])
            for n, (j, at, to) in enumerate(spots):
                m.append(jnp.maximum(top[to, :], row_max(oth[n])))
            for n, (j, at, to) in enumerate(spots):
                oth[n] = jnp.exp(oth[n] - jnp.concatenate([m[n]] * (far // HEAD), axis=1))
                keep.append(jnp.exp(top[to, :] - m[n]))
            for n, (j, at, to) in enumerate(spots):
                inv.append(1.0 / (low[to, :] * keep[n] + row_sum(oth[n])))
            for n, (j, at, to) in enumerate(spots):
                mixed = acc[to, :] * keep[n] + dot(oth[n].astype(BF), kv[n, :, HEAD:])
                mixed = (mixed * inv[n]).astype(BF)
                out[pl.ds(at, QB), :HEAD] = mixed[:QB]
                out[pl.ds(at, QB), HEAD:] = mixed[QB:]
            return carry

        lax.fori_loop(0, q.shape[0] // QB // GROUP, step, 0)

    return body


def attend_early(want, bias, q, held, recv):
    counts = [r[0].shape[0] for r in recv]
    ins = [*held, *[a for r in recv for a in r]]
    rows = 2 * q.shape[0]
    return pl.pallas_call(
        early_body(counts),
        out_shape=[
            jax.ShapeDtypeStruct((rows, HEAD), F32),
            jax.ShapeDtypeStruct((rows, HEAD), F32),
            jax.ShapeDtypeStruct((rows, HEAD), F32),
        ],
        in_specs=[SMEM] + [VMEM] * (2 + len(ins)),
        out_specs=[VMEM] * 3,
        scratch_shapes=[pltpu.VMEM((GROUP, sum(counts) * NX * KB, 2 * HEAD), BF)],
        compiler_params=params(16),
        cost_estimate=pl.CostEstimate(
            flops=900_000_000, bytes_accessed=6_000_000, transcendentals=1_600_000
        ),
        name="early",
    )(want, bias, q, *ins)


def attend_late(want, bias, q, sums, held, recv):
    counts = [r[0].shape[0] for r in recv]
    first = bias.shape[1] // (NX * KB) - sum(counts)
    ins = [*held, *[a for r in recv for a in r]]
    return pl.pallas_call(
        late_body(counts, first),
        out_shape=jax.ShapeDtypeStruct(q.shape, BF),
        in_specs=[SMEM] + [VMEM] * (2 + len(sums) + len(ins)),
        out_specs=VMEM,
        scratch_shapes=[pltpu.VMEM((GROUP, sum(counts) * NX * KB, 2 * HEAD), BF)],
        compiler_params=params(16),
        cost_estimate=pl.CostEstimate(
            flops=400_000_000, bytes_accessed=6_000_000, transcendentals=800_000
        ),
        name="late",
    )(want, bias, q, *sums, *ins)


def project_body(spot, att, *refs):
    count = 2 * NY
    weights, (out, near, acc, sems) = refs[:count], refs[count:]
    copies = [pltpu.make_async_copy(w, near.at[i], sems.at[i]) for i, w in enumerate(weights)]
    for c in copies:
        c.start()
    tile = 512
    for i, c in enumerate(copies):
        c.wait()
        mine = att[spot[i // NY, i % NY]]
        for n in range(out.shape[1] // tile):
            cols = slice(n * tile, (n + 1) * tile)
            part = dot(mine, near[i, :, cols]).astype(BF).astype(F32)
            if i == 0:
                acc[:, cols] = part
            elif i < count - 1:
                acc[:, cols] += part
            else:
                out[:, cols] = (acc[:, cols] + part).astype(BF)


def project(spot, att, weights):
    deep, width = weights[0].shape
    return pl.pallas_call(
        project_body,
        out_shape=jax.ShapeDtypeStruct((QB, width), BF),
        in_specs=[SMEM, VMEM] + [ANY] * len(weights),
        out_specs=VMEM,
        scratch_shapes=[
            pltpu.VMEM((len(weights), deep, width), BF),
            pltpu.VMEM((QB, width), F32),
            pltpu.SemaphoreType.DMA((len(weights),)),
        ],
        compiler_params=params(14),
        cost_estimate=pl.CostEstimate(
            flops=1_000_000_000, bytes_accessed=9_000_000, transcendentals=0
        ),
        name="project",
    )(spot, att, *weights)


def layer(tokens, wq, wk, wv, wo, chosen):
    me = lax.axis_index("kv")
    z, x = me // NX, me % NX
    tp = lax.axis_index("tp")
    per = tokens.shape[0] // KB

    kv = rows_project(tokens, (wk, wv), 60)

    row = jnp.stack([chosen] + [lax.ppermute(chosen, "kv", along_x(-r)) for r in range(1, NX)])

    order = [0, *[d for s in range(1, NZ // 2) for d in (s, NZ - s)], NZ // 2]

    def wants(lists, dist):
        groups = (z - np.repeat(np.array(dist, np.int32), chosen.shape[0])) % NZ * NX + x
        named = jnp.concatenate([lists] * len(dist), axis=1)
        mine = named // per == groups[None, :, None]
        return jnp.sum(jnp.where(mine, named % per, 0), axis=2)

    want = wants(row, order)
    dist = np.repeat(np.array(order, np.int32), NX * KB)
    beyond = np.tile(np.repeat(np.arange(NX, dtype=np.int32), KB), NZ)
    source = (z - dist) % NZ * NX + (x - beyond) % NX
    groups = chosen // per
    here = groups[:, :1] == source[None, :]
    for n in range(1, NFAR):
        here = here | (groups[:, n : n + 1] == source[None, :])
    bias = jnp.where(here, 0.0, -jnp.inf).astype(F32)

    held = {0: kv}
    up = down = kv
    for step in range(1, NZ // 2 + 1):
        up = held[step] = lax.ppermute(up, "kv", along_z(1))
        if step < NZ // 2:
            down = held[NZ - step] = lax.ppermute(down, "kv", along_z(-1))

    recv = []
    batches = [[0, 1, NZ - 1]] + [[s, NZ - s] for s in range(2, NZ // 2)] + [[NZ // 2]]
    beside = range(1, NX)
    for batch in batches:
        sent = pick(want, order.index(batch[0]), [held[d] for d in batch], beside)
        recv.append([lax.ppermute(a, "kv", along_x(r)) for a, r in zip(sent, beside)])
    wm = lax.ppermute(wo, "tp", along_y(1))
    wp = lax.ppermute(wo, "tp", along_y(-1))
    weights = [wo, wm, wp, lax.ppermute(wm, "tp", along_y(1))]
    weights += [lax.ppermute(w, "tp", CORES) for w in weights]

    q = rows_project(tokens, (wq,), 60)
    line = [held[d] for d in order]
    cut = len(batches[0]) + len(batches[1])
    sums = attend_early(want, bias, q, line[:cut], recv[:2])
    mixed = attend_late(want, bias, q, sums, line[cut:], recv[2:])
    att = lax.all_to_all(mixed.reshape(2 * NY, QB, -1), "tp", 0, 0, tiled=True)
    y, c = tp // 2, tp % 2
    rows = jnp.stack([y, (y - 1) % NY, (y + 1) % NY, (y + 2) % NY]) * 2
    return project(jnp.stack([rows + c, rows + 1 - c]), att, weights)


def solution(mesh):
    return jax.shard_map(
        layer,
        mesh=mesh,
        in_specs=(
            P("kv", None),
            P(None, "tp"),
            P(None, "tp"),
            P(None, "tp"),
            P("tp", None),
            P("kv", None),
        ),
        out_specs=P(("kv", "tp"), None),
        check_vma=False,
    )
```

```python
import jax
import jax.numpy as jnp
import numpy as np
from jax import lax
from jax.experimental import pallas as pl
from jax.experimental.pallas import tpu as pltpu
from jax.sharding import PartitionSpec as P

HEAD = 128
QB = 128
KB = 32
NFAR = 12
NX = 4
NZ = 8
NY = 4
GROUP = 4
BF = jnp.bfloat16
F32 = jnp.float32
NT = (((1,), (1,)), ((), ()))


CORES = [(t, t ^ 1) for t in range(2 * NY)]


def along_z(k):
    return [(z * NX + x, (z + k) % NZ * NX + x) for z in range(NZ) for x in range(NX)]


def along_x(k):
    return [(z * NX + x, z * NX + (x + k) % NX) for z in range(NZ) for x in range(NX)]


def along_y(k):
    return [(y * 2 + c, (y + k) % NY * 2 + c) for y in range(NY) for c in range(2)]


def dot(a, b):
    return jnp.dot(a, b, preferred_element_type=F32)


VMEM = pl.BlockSpec(memory_space=pltpu.VMEM)
SMEM = pl.BlockSpec(memory_space=pltpu.SMEM)
ANY = pl.BlockSpec(memory_space=pl.ANY)


def params(mib):
    return pltpu.CompilerParams(vmem_limit_bytes=mib * 1024 * 1024)


def rows_body(count, parts):
    def body(tok, *refs):
        weights, (out, t, w, sems) = refs[:count], refs[count:]
        tile = out.shape[0] // parts
        wide = out.shape[1] // count
        copies = [
            pltpu.make_async_copy(ref, w.at[:, pl.ds(n * wide, wide)], sems.at[n])
            for n, ref in enumerate(weights)
        ]
        blocks = [pl.ds(n * tile, tile) for n in range(parts)]
        copies += [
            pltpu.make_async_copy(tok.at[b], t.at[b], sems.at[count + n]) for n, b in enumerate(blocks)
        ]
        for c in copies:
            c.start()
        for c in copies[:count]:
            c.wait()
        for c, b in zip(copies[count:], blocks):
            c.wait()
            out[b, :] = dot(t[b, :], w[...]).astype(BF)

    return body


def rows_project(tokens, weights, limit):
    rows, width = tokens.shape
    parts = 4
    total = sum(w.shape[1] for w in weights)
    return pl.pallas_call(
        rows_body(len(weights), parts),
        out_shape=jax.ShapeDtypeStruct((rows, total), BF),
        in_specs=[ANY] * (1 + len(weights)),
        out_specs=VMEM,
        scratch_shapes=[
            pltpu.VMEM((rows, width), BF),
            pltpu.VMEM((width, total), BF),
            pltpu.SemaphoreType.DMA((len(weights) + parts,)),
        ],
        compiler_params=params(limit),
        cost_estimate=pl.CostEstimate(
            flops=1_000_000_000, bytes_accessed=6_000_000, transcendentals=0
        ),
    )(tokens, *weights)


def pick_body(first, count, offsets):
    def body(want, *refs):
        ins, outs = refs[:count], refs[count:]

        def step(j, carry):
            for d in range(count):
                for out, r in zip(outs, offsets):
                    b = pl.multiple_of(want[r, (first + d) * 8 + j] * KB, KB)
                    out[d, j] = ins[d][pl.ds(b, KB), :]
            return carry

        lax.fori_loop(0, 8, step, 0)

    return body


def pick(want, first, held, offsets):
    count = len(held)
    return pl.pallas_call(
        pick_body(first, count, offsets),
        out_shape=[jax.ShapeDtypeStruct((count, 8, KB, 2 * HEAD), BF)] * len(offsets),
        in_specs=[SMEM] + [VMEM] * count,
        out_specs=[VMEM] * len(offsets),
        compiler_params=params(6),
        cost_estimate=pl.CostEstimate(
            flops=4_000_000 * count, bytes_accessed=1_000_000 * count, transcendentals=0
        ),
    )(want, *held)


def gather_blocks(kv, want, held, recv, counts, first, j):
    slot = 0
    source = 0

    def put(block):
        nonlocal slot
        kv[slot * KB : (slot + 1) * KB, :] = block
        slot += 1

    for b, count in enumerate(counts):
        for d in range(count):
            mine = pl.multiple_of(want[0, (first + source) * 8 + j] * KB, KB)
            put(held[source][pl.ds(mine, KB), :])
            for r in range(1, NX):
                put(recv[(NX - 1) * b + r - 1][d, j])
            source += 1


def both_heads(q, at):
    return jnp.concatenate([q[pl.ds(at, QB), :HEAD], q[pl.ds(at, QB), HEAD:]], axis=0)


def row_max(a):
    return jnp.max(a, axis=1, keepdims=True)


def row_sum(a):
    return jnp.sum(a, axis=1, keepdims=True)


def places(j):
    return j, pl.multiple_of(j * QB, QB), pl.ds(pl.multiple_of(j * 2 * QB, 2 * QB), 2 * QB)


def early_body(counts):
    total = sum(counts)
    far = total * NX * KB

    def body(want, bias, q, *refs):
        held, recv = refs[:total], refs[total:-4]
        acc, top, low, kv = refs[-4:]
        row = lax.broadcasted_iota(jnp.int32, (2 * QB, QB), 0) % QB
        col = lax.broadcasted_iota(jnp.int32, (2 * QB, QB), 1)
        causal = jnp.where(col <= row, 0.0, -jnp.inf).astype(F32)
        scale = HEAD ** (-0.5)

        def step(g, carry):
            spots = [places(g * GROUP + n) for n in range(GROUP)]
            own, oth, m = [], [], []
            for n, (j, at, to) in enumerate(spots):
                gather_blocks(kv.at[n], want, held, recv, counts, 0, j)
            for n, (j, at, to) in enumerate(spots):
                qq = both_heads(q, at)
                mine = held[0][pl.ds(at, QB), :HEAD]
                own.append(lax.dot_general(qq, mine, NT, preferred_element_type=F32) * scale + causal)
                theirs = kv[n, :, :HEAD]
                oth.append(
                    lax.dot_general(qq, theirs, NT, preferred_element_type=F32) * scale
                    + bias[pl.ds(j, 1), :far]
                )
            for n in range(GROUP):
                m.append(jnp.maximum(row_max(own[n]), row_max(oth[n])))
            for n in range(GROUP):
                own[n] = jnp.exp(own[n] - m[n])
                oth[n] = jnp.exp(oth[n] - m[n])
            for n, (j, at, to) in enumerate(spots):
                top[to, :] = jnp.broadcast_to(m[n], (2 * QB, HEAD))
                low[to, :] = jnp.broadcast_to(row_sum(own[n]) + row_sum(oth[n]), (2 * QB, HEAD))
                mixed = dot(own[n].astype(BF), held[0][pl.ds(at, QB), HEAD:])
                acc[to, :] = mixed + dot(oth[n].astype(BF), kv[n, :, HEAD:])
            return carry

        lax.fori_loop(0, q.shape[0] // QB // GROUP, step, 0)

    return body


def late_body(counts, first):
    total = sum(counts)

    def body(want, turn, bias, q, acc, top, low, *refs):
        held, recv = refs[:total], refs[total:-3]
        kv = refs[-1]
        begin = first * NX * KB
        far = kv.shape[1]
        scale = HEAD ** (-0.5)

        def step(out, other):
            y, c = turn[0] // 2, turn[0] % 2
            c = 1 - c if other else c
            spots = [places((y + n) % NY * 2 + c) for n in range(NY)]
            oth, m, keep, inv = [], [], [], []
            for n, (j, at, to) in enumerate(spots):
                gather_blocks(kv.at[n], want, held, recv, counts, first, j)
            for n, (j, at, to) in enumerate(spots):
                part = lax.dot_general(both_heads(q, at), kv[n, :, :HEAD], NT, preferred_element_type=F32)
                oth.append(part * scale + bias[pl.ds(j, 1), begin : begin + far])
            for n, (j, at, to) in enumerate(spots):
                m.append(jnp.maximum(top[to, :], row_max(oth[n])))
            for n, (j, at, to) in enumerate(spots):
                oth[n] = jnp.exp(oth[n] - jnp.concatenate([m[n]] * (far // HEAD), axis=1))
                keep.append(jnp.exp(top[to, :] - m[n]))
            for n, (j, at, to) in enumerate(spots):
                inv.append(1.0 / (low[to, :] * keep[n] + row_sum(oth[n])))
            for n, (j, at, to) in enumerate(spots):
                mixed = acc[to, :] * keep[n] + dot(oth[n].astype(BF), kv[n, :, HEAD:])
                mixed = (mixed * inv[n]).astype(BF)
                out[n, :, :HEAD] = mixed[:QB]
                out[n, :, HEAD:] = mixed[QB:]

        step(refs[-2], True)
        step(refs[-3], False)

    return body


def attend_early(want, bias, q, held, recv):
    counts = [r[0].shape[0] for r in recv]
    ins = [*held, *[a for r in recv for a in r]]
    rows = 2 * q.shape[0]
    return pl.pallas_call(
        early_body(counts),
        out_shape=[
            jax.ShapeDtypeStruct((rows, HEAD), F32),
            jax.ShapeDtypeStruct((rows, HEAD), F32),
            jax.ShapeDtypeStruct((rows, HEAD), F32),
        ],
        in_specs=[SMEM] + [VMEM] * (2 + len(ins)),
        out_specs=[VMEM] * 3,
        scratch_shapes=[pltpu.VMEM((GROUP, sum(counts) * NX * KB, 2 * HEAD), BF)],
        compiler_params=params(16),
        cost_estimate=pl.CostEstimate(
            flops=900_000_000, bytes_accessed=6_000_000, transcendentals=1_600_000
        ),
        name="early",
    )(want, bias, q, *ins)


def attend_late(want, turn, bias, q, sums, held, recv):
    counts = [r[0].shape[0] for r in recv]
    first = bias.shape[1] // (NX * KB) - sum(counts)
    ins = [*held, *[a for r in recv for a in r]]
    return pl.pallas_call(
        late_body(counts, first),
        out_shape=[jax.ShapeDtypeStruct((NY, QB, 2 * HEAD), BF)] * 2,
        in_specs=[SMEM] * 2 + [VMEM] * (2 + len(sums) + len(ins)),
        out_specs=[VMEM] * 2,
        scratch_shapes=[pltpu.VMEM((NY, sum(counts) * NX * KB, 2 * HEAD), BF)],
        compiler_params=params(16),
        cost_estimate=pl.CostEstimate(
            flops=400_000_000, bytes_accessed=6_000_000, transcendentals=800_000
        ),
        name="late",
    )(want, turn, bias, q, *sums, *ins)


def pack_body(mine, theirs, *outs):
    for n, out in enumerate(outs):
        out[0] = mine[n + 1]
        out[1] = theirs[n + 1]


def pack(mine, theirs):
    return pl.pallas_call(
        pack_body,
        out_shape=[jax.ShapeDtypeStruct((2, *mine.shape[1:]), BF)] * (NY - 1),
        in_specs=[VMEM] * 2,
        out_specs=[VMEM] * (NY - 1),
        compiler_params=params(4),
        cost_estimate=pl.CostEstimate(flops=1_000_000, bytes_accessed=800_000, transcendentals=0),
        name="pack",
    )(mine, theirs)


def stage_body(*refs):
    out, sems = refs[-2:]
    copies = [pltpu.make_async_copy(ref, out.at[n], sems.at[n]) for n, ref in enumerate(refs[:-2])]
    run_all(copies)


def run_all(copies):
    for c in copies:
        c.start()
    for c in copies:
        c.wait()


def stage(weights):
    return pl.pallas_call(
        stage_body,
        out_shape=jax.ShapeDtypeStruct((len(weights), *weights[0].shape), BF),
        in_specs=[ANY] * len(weights),
        out_specs=VMEM,
        scratch_shapes=[pltpu.SemaphoreType.DMA((len(weights),))],
        compiler_params=params(10),
        cost_estimate=pl.CostEstimate(flops=1_000_000_000, bytes_accessed=16_000_000, transcendentals=0),
        name="stage",
    )(*weights)


def project_body(mine, theirs, *refs):
    others, (weights, out) = refs[:-2], refs[-2:]
    left = [mine[0], *[a[0] for a in others], theirs[0], *[a[1] for a in others]]
    tile = 512
    for n in range(out.shape[1] // tile):
        cols = slice(n * tile, (n + 1) * tile)
        acc = None
        for i, a in enumerate(left):
            part = dot(a, weights[i, :, cols]).astype(BF).astype(F32)
            acc = part if acc is None else acc + part
        out[:, cols] = acc.astype(BF)


def project(mine, theirs, others, weights):
    return pl.pallas_call(
        project_body,
        out_shape=jax.ShapeDtypeStruct((QB, weights.shape[2]), BF),
        in_specs=[VMEM] * (3 + len(others)),
        out_specs=VMEM,
        compiler_params=params(10),
        cost_estimate=pl.CostEstimate(
            flops=1_000_000_000, bytes_accessed=9_000_000, transcendentals=0
        ),
        name="project",
    )(mine, theirs, *others, weights)


def layer(tokens, wq, wk, wv, wo, chosen):
    me = lax.axis_index("kv")
    z, x = me // NX, me % NX
    tp = lax.axis_index("tp")
    per = tokens.shape[0] // KB

    kv = rows_project(tokens, (wk, wv), 60)

    kv, turn = lax.optimization_barrier((kv, tp.reshape(1)))

    row = jnp.stack([chosen] + [lax.ppermute(chosen, "kv", along_x(-r)) for r in range(1, NX)])

    order = [0, *[d for s in range(1, NZ // 2) for d in (s, NZ - s)], NZ // 2]

    def wants(lists, dist):
        groups = (z - np.repeat(np.array(dist, np.int32), chosen.shape[0])) % NZ * NX + x
        named = jnp.concatenate([lists] * len(dist), axis=1)
        mine = named // per == groups[None, :, None]
        return jnp.sum(jnp.where(mine, named % per, 0), axis=2)

    want = wants(row, order)
    dist = np.repeat(np.array(order, np.int32), NX * KB)
    beyond = np.tile(np.repeat(np.arange(NX, dtype=np.int32), KB), NZ)
    source = (z - dist) % NZ * NX + (x - beyond) % NX
    groups = chosen // per
    here = groups[:, :1] == source[None, :]
    for n in range(1, NFAR):
        here = here | (groups[:, n : n + 1] == source[None, :])
    bias = jnp.where(here, 0.0, -jnp.inf).astype(F32)

    held = {0: kv}
    up = down = kv
    for step in range(1, NZ // 2 + 1):
        up = held[step] = lax.ppermute(up, "kv", along_z(1))
        if step < NZ // 2:
            down = held[NZ - step] = lax.ppermute(down, "kv", along_z(-1))

    recv = []
    batches = [[0, 1, NZ - 1]] + [[s, NZ - s] for s in range(2, NZ // 2)] + [[NZ // 2]]
    beside = range(1, NX)
    for batch in batches:
        sent = pick(want, order.index(batch[0]), [held[d] for d in batch], beside)
        recv.append([lax.ppermute(a, "kv", along_x(r)) for a, r in zip(sent, beside)])
    wm = lax.ppermute(wo, "tp", along_y(1))
    wp = lax.ppermute(wo, "tp", along_y(-1))
    weights = [wo, wm, lax.ppermute(wm, "tp", along_y(1)), wp]
    weights += [lax.ppermute(w, "tp", CORES) for w in weights]

    q = rows_project(tokens, (wq,), 60)
    line = [held[d] for d in order]
    cut = len(batches[0]) + len(batches[1])
    sums = attend_early(want, bias, q, line[:cut], recv[:2])
    mine, cross = attend_late(want, turn, bias, q, sums, line[cut:], recv[2:])
    theirs = lax.ppermute(cross, "tp", CORES)
    others = [lax.ppermute(a, "tp", along_y(n + 1)) for n, a in enumerate(pack(mine, theirs))]
    return project(mine, theirs, others, stage(weights))


def solution(mesh):
    return jax.shard_map(
        layer,
        mesh=mesh,
        in_specs=(
            P("kv", None),
            P(None, "tp"),
            P(None, "tp"),
            P(None, "tp"),
            P("tp", None),
            P("kv", None),
        ),
        out_specs=P(("kv", "tp"), None),
        check_vma=False,
    )
```
